32 devices in a mesh: grp: 2 (over y), fs: 4 (over z), tp: 4 (over x, core).
Axes of the slice: x: 2, y: 2, z: 4, core: 2. Of those that a mesh axis runs over, the one named last changes fastest.
Arguments:
- tokens: bfloat16 [1536, 2048], P(('grp', 'tp')), parts along dimension 0, may hold values from -6 to 6
- routes: int32 [1536, 2], P(('grp', 'tp')), parts along dimension 0, may hold values from 0 to 3, all different within a row; in each aligned block of 192 rows (0 to 191, 192 to 383, ...) at most 128 rows name the same one
- route_weight: float32 [1536, 2], P(('grp', 'tp')), parts along dimension 0, may hold values from 0.2 to 1
- norm_gain: float32 [2048], P('fs'), may hold values from 0.1 to 1.9
- gate_train: float32 [4, 2048, 5632], P('tp', 'fs'), may hold values from -0.125 to 0.125
- up_train: float32 [4, 2048, 5632], P('tp', 'fs'), may hold values from -0.125 to 0.125
- down_train: float32 [4, 5632, 2048], P('tp', None, 'fs'), may hold values from -0.109375 to 0.109375
Outputs:
- gate_serve: bfloat16 [8, 2048, 5632], P(('grp', 'tp'), None, 'fs'), parts along dimension 0
- up_serve: bfloat16 [8, 2048, 5632], P(('grp', 'tp'), None, 'fs'), parts along dimension 0
- down_serve: bfloat16 [8, 5632, 2048], P(('grp', 'tp'), 'fs'), parts along dimension 0
- mixed: bfloat16 [1536, 2048], P(('grp', 'tp'), 'fs'), parts along dimension 0
The draws below stay inside these ranges and needn't reach their ends.
There are 2 independent parts, one for each index of `grp`. The reference program is written for one: setup_inputs(seed, part) draws one part's arguments, and reference() takes and returns one part's arrays. A program takes and returns all parts, laid end to end along the dimension named above; an argument that names none is the same for every part. Nothing has to cross between parts.
Inputs may be any that keep to these rules, and one draw needn't show every extreme that they name: `routes`: each row names 2 different experts. In each aligned block of 192 rows no expert is named by more than 128 rows, a bound that some block reaches.
All inputs are finite; a program needn't handle non-finite values.
Results may differ from the reference program's by a relative error of at most 0.0087.
Values may be sent and summed in bfloat16 or wider, within the bound.
A program may use at most 128 MiB of HBM per device.

```python
import math
import jax
import jax.numpy as jnp
import numpy as np
from jax import lax

D = 2048
FF = 5632
EXPERTS = 4
TOP = 2
TOK_DEV = 192
CAP = 128
TOKENS = 768
COPIES = 1


def strengthened(values, own_key, source, target, blocks, factor):
    def block_of(axis_at):
        return (jnp.arange(values.shape[axis_at]) // (values.shape[axis_at] // blocks)).reshape((-1,) + (1,) * (values.ndim - 1 - axis_at))

    one_side = jax.random.permutation(own_key, blocks)[block_of(target)]
    other_side = (block_of(target) + blocks // 2) % blocks
    return jnp.where((block_of(source) == one_side) | (block_of(source) == other_side), factor * values, values)


def levels(key, extent, pieces, least, largest):
    loudness = 1.0
    for dim, blocks in pieces:
        draws = jax.random.uniform(jax.random.fold_in(jax.random.fold_in(key, 6), dim), (blocks,), jnp.float32, least / len(pieces), largest / len(pieces))
        loudness = loudness * jnp.repeat(jnp.exp(draws), extent[dim] // blocks).reshape((-1,) + (1,) * (len(extent) - 1 - dim))
    return loudness


def routed_block(own_key, own, number, rows, count, top, bound, lean):
    order = jax.random.permutation(own_key, count)
    packed, usual = portions_of(count, rows * top, bound, lean, True), portions_of(count, rows * top, bound, lean, False)
    places = jnp.arange(count)

    def named(lengths, turn):
        used = int((lengths > 0).sum())
        fixed = max(1, used // 4)
        moved = fixed + (places - fixed + turn * (used - fixed)) % max(1, count - fixed)
        return jnp.zeros((count,), jnp.int32).at[order[jnp.where(places < fixed, places, moved)]].set(jnp.asarray(lengths, jnp.int32))

    lengths = jnp.where(number % 4 == 0, named(packed, number // 4), named(usual, number - number // 4 - 1))
    mixed = jax.random.permutation(jax.random.fold_in(own, 3), count)
    giver, sink = mixed[0:count // 2 * 2:2], mixed[1:count // 2 * 2:2]
    slack = jnp.minimum(lengths[giver] - 1, bound - lengths[sink]) // 2
    slack = jnp.where((giver == order[0]) | (sink == order[0]) | (lengths[sink] == 0), 0, jnp.maximum(slack, 0))
    moved = jax.random.randint(jax.random.fold_in(own, 4), (count // 2,), 0, 1 << 20) % (slack + 1)
    lengths = lengths.at[giver].add(-moved).at[sink].add(moved)
    items = jnp.searchsorted(jnp.cumsum(lengths), jnp.arange(rows * top), side="right").astype(jnp.int32)
    table = items.reshape(top, rows).T
    table = table[jax.random.permutation(jax.random.fold_in(own, 1), rows)]
    turn = jax.random.randint(jax.random.fold_in(own, 2), (rows, 1), 0, top)
    return jnp.take_along_axis(table, (jnp.arange(top)[None, :] + turn) % top, axis=1)


def portions_of(amount, total, limit, slope, full):
    weights = [(1 << 20) // math.isqrt(grade ** slope) + 1 for grade in range(1, amount + 1)]
    largest = limit if full else min(limit, max(-(-total // amount), total * weights[0] // sum(weights)))
    least = 1 if total - largest >= amount - 1 else 0
    holding, rest = [largest] + [least] * (amount - 1), total - largest - least * (amount - 1)
    while rest > 0:
        movable = [i for i in range(1, amount) if holding[i] < largest] or [i for i in range(1, amount) if holding[i] < limit]
        whole, left = sum([weights[i] for i in movable]), rest
        for i in movable:
            extra = min(limit - holding[i], max(1, left * weights[i] // whole), rest)
            holding[i] = holding[i] + extra
            rest = rest - extra
    return np.array(holding)


def gaussian(key, shape, width, limit, pieces=(), kind=jnp.bfloat16):
    values = jax.random.normal(key, shape, jnp.float32) * width
    if len(pieces) > 0:
        values = levels(key, shape, pieces, -0.22, 0.18) * values
    return jnp.clip(values, min=-limit, max=limit).astype(kind)


def gaussian_with(stream_key, dims, spread, most, split, heavy, held_as=jnp.bfloat16):
    drawn = spread * jax.random.normal(stream_key, dims, jnp.float32)
    if split:
        drawn = drawn * levels(stream_key, dims, split, -0.22, 0.18)
    return jnp.clip(strengthened(drawn, jax.random.fold_in(stream_key, 3), *heavy), -most, most).astype(held_as)


def setup_inputs(seed: int = 0, part: int = 0) -> dict:
    streams_of = jax.random.split(jax.random.key(seed), 8)
    part_splits = jax.random.split(jax.random.fold_in(streams_of[7], part), 8)
    tokens = gaussian(part_splits[0], (TOKENS, D), 1.0, 6.0, ((0, 4),))
    routes_keys = jax.random.split(jax.random.fold_in(part_splits[1], 1), TOKENS // TOK_DEV)
    routes_turns = jax.random.permutation(jax.random.fold_in(part_splits[1], 3), TOKENS // TOK_DEV)
    routes = jax.vmap(lambda own, number: routed_block(jax.random.fold_in(part_splits[1], 2), own, number, TOK_DEV, EXPERTS, TOP, CAP, 1))(routes_keys, routes_turns).reshape((TOKENS, TOP))
    route_weight = jnp.clip(0.2 + 0.8 * jax.random.uniform(part_splits[2], (TOKENS, TOP), jnp.float32) ** levels(part_splits[2], (TOKENS, TOP), ((0, 4),), -0.2, 0.2), 0.2, 1.0)
    norm_gain = jnp.clip(1.0 + 0.18 * jax.random.normal(streams_of[3], (D,), jnp.float32), 0.1, 1.9)
    gate_train = gaussian(streams_of[4], (EXPERTS, D, FF), D ** -0.5, 0.125, ((0, 4), (1, 4)), jnp.float32)
    up_train = gaussian(streams_of[5], (EXPERTS, D, FF), D ** -0.5, 0.125, ((0, 4), (1, 4)), jnp.float32)
    down_train = gaussian_with(streams_of[6], (EXPERTS, FF, D), FF ** -0.5, 0.109375, ((0, 4), (2, 4)), (1, 2, 4, 2.0), jnp.float32)
    return {"tokens": tokens, "routes": routes, "route_weight": route_weight, "norm_gain": norm_gain, "gate_train": gate_train, "up_train": up_train, "down_train": down_train}


def reference(tokens, routes, route_weight, norm_gain, gate_train, up_train, down_train):
    gain_column = norm_gain[None, :, None]
    gate_low = (gate_train * gain_column).astype(jnp.bfloat16)
    up_low = (up_train * gain_column).astype(jnp.bfloat16)
    down_low = down_train.astype(jnp.bfloat16)
    tok_float = tokens.astype(jnp.float32)
    normed = (tok_float * lax.rsqrt(lax.optimization_barrier(jnp.mean(tok_float * tok_float, axis=-1, keepdims=True)) + 1e-06)).astype(jnp.bfloat16)
    normed_wide = normed.astype(jnp.float32)

    def expert(triple):
        gate_one, up_one, down_one = triple
        gated = jnp.dot(normed_wide, gate_one.astype(jnp.float32), preferred_element_type=jnp.float32)
        lifted = jnp.dot(normed_wide, up_one.astype(jnp.float32), preferred_element_type=jnp.float32)
        hidden = (jax.nn.silu(gated) * lifted).astype(jnp.bfloat16)
        return jnp.dot(hidden.astype(jnp.float32), down_one.astype(jnp.float32), preferred_element_type=jnp.float32).astype(jnp.bfloat16)
    outputs = lax.map(expert, (gate_low, up_low, down_low))
    row_index = jnp.arange(tokens.shape[0], dtype=jnp.int32)
    first = outputs[routes[:, 0], row_index].astype(jnp.float32)
    second = outputs[routes[:, 1], row_index].astype(jnp.float32)
    mixed = route_weight[:, 0:1] * first + route_weight[:, 1:2] * second
    gate_serve = jnp.tile(gate_low, (1, 1, COPIES))
    up_serve = jnp.tile(up_low, (1, 1, COPIES))
    down_serve = jnp.tile(down_low, (1, COPIES, 1))
    return (gate_serve, up_serve, down_serve, mixed.astype(jnp.bfloat16))
```

```python
import functools
import jax
import jax.numpy as jnp
from jax import lax
from jax.experimental import pallas as pl
from jax.experimental.pallas import tpu as pltpu
from jax.sharding import PartitionSpec as P

EXPERTS = 4
CAP = 128
MESH = pl.DeviceIdType.MESH


def exchange_kernel(F, T, R, C, gl, ul, dl, xs, bh, bl, go, uo, do, mo,
                    gw, uw, dw, arr, gacc, uacc, hid, pbf, ret, msend, mown, mrecv,
                    zs, zr, ys, yr, ts, tr, ps, pr, ms, mr, loc, xloc, osem):
    g, f, t = lax.axis_index("grp"), lax.axis_index("fs"), lax.axis_index("tp")
    H = R // 2
    lows, wins, outs = (gl, ul, dl), (gw, uw, dw), (go, uo, do)
    half_f = F // 2
    lo = lax.div(f, half_f)
    peers = [lax.rem(t + d, T) for d in range(1, T)]
    others = [lo * k + (1 - lo) * (F - 1 - k) for k in range(half_f)]
    others += [lo * half_f + lax.rem(f - lo * half_f + 1 + j, half_f) for j in range(half_f - 1)]

    barrier = pltpu.get_barrier_semaphore()
    for p in peers:
        pl.semaphore_signal(barrier, inc=1, device_id={"tp": p}, device_id_type=MESH)
    for p in others:
        pl.semaphore_signal(barrier, inc=1, device_id={"fs": p}, device_id_type=MESH)
    pl.semaphore_signal(barrier, inc=1, device_id={"grp": 1 - g}, device_id_type=MESH)
    pl.semaphore_wait(barrier, len(peers) + len(others) + 1)

    def cols_of(src, half):
        return pl.ds(pl.multiple_of(src * R + half * H, H), H)

    def part(a, src, half):
        if a < 2:
            return wins[a].at[cols_of(src, half), :]
        return dw.at[:, cols_of(src, half)]

    def z_copy(a, tgt, src):
        if a < 2:
            piece = lows[a].at[pl.ds(pl.multiple_of(g * H, H), H), pl.ds(pl.multiple_of(tgt * C, C), C)]
        else:
            piece = dl.at[pl.ds(pl.multiple_of(tgt * C, C), C), pl.ds(pl.multiple_of(g * H, H), H)]
        return pltpu.make_async_remote_copy(
            src_ref=piece, dst_ref=part(a, src, g), send_sem=zs.at[a, tgt], recv_sem=zr.at[a, src],
            device_id={"fs": tgt}, device_id_type=MESH)

    def z_recv(a, src):
        return pltpu.make_async_remote_copy(
            src_ref=part(a, src, g), dst_ref=part(a, src, g), send_sem=zs.at[a, src], recv_sem=zr.at[a, src],
            device_id={"fs": src}, device_id_type=MESH)

    def y_copy(a, src, half):
        return pltpu.make_async_remote_copy(
            src_ref=part(a, src, half), dst_ref=part(a, src, half), send_sem=ys.at[a, src], recv_sem=yr.at[a, src],
            device_id={"grp": 1 - g}, device_id_type=MESH)

    def slots(q):
        return pl.ds(pl.multiple_of(q * CAP, CAP), CAP)

    def t_copy(tgt, src):
        return pltpu.make_async_remote_copy(
            src_ref=xs.at[tgt], dst_ref=arr.at[slots(src), :], send_sem=ts.at[tgt], recv_sem=tr.at[src],
            device_id={"tp": tgt}, device_id_type=MESH)

    def p_copy(c, half, tgt, src):
        cols = cols_of(c, half)
        return pltpu.make_async_remote_copy(
            src_ref=pbf.at[slots(tgt), cols], dst_ref=ret.at[slots(src), cols],
            send_sem=ps.at[c, half, tgt], recv_sem=pr.at[c, half, src],
            device_id={"tp": tgt}, device_id_type=MESH)

    def m_copy(tgt, half, src):
        return pltpu.make_async_remote_copy(
            src_ref=msend.at[:, cols_of(tgt, half)], dst_ref=mrecv.at[src, :, pl.ds(pl.multiple_of(half * H, H), H)],
            send_sem=ms.at[tgt, half], recv_sem=mr.at[src, half],
            device_id={"fs": tgt}, device_id_type=MESH)

    def own_copy(a):
        if a < 2:
            return pltpu.make_async_copy(lows[a].at[:, pl.ds(pl.multiple_of(f * C, C), C)],
                                         wins[a].at[pl.ds(pl.multiple_of(f * R, R), R), :], loc.at[a])
        return pltpu.make_async_copy(dl.at[pl.ds(pl.multiple_of(f * C, C), C), :],
                                     dw.at[:, pl.ds(pl.multiple_of(f * R, R), R)], loc.at[a])

    def out_copy(a, src):
        whole = pl.ds(pl.multiple_of(src * R, R), R)
        if a < 2:
            return pltpu.make_async_copy(wins[a].at[whole, :], outs[a].at[whole, :], osem.at[a, src])
        return pltpu.make_async_copy(dw.at[:, whole], do.at[:, whole], osem.at[a, src])

    for p in peers:
        t_copy(p, t).start()
    for a in (0, 1):
        for p in others:
            z_copy(a, p, f).start()
    for p in others:
        z_copy(2, p, f).start()
    own_x = pltpu.make_async_copy(xs.at[t], arr.at[slots(t), :], xloc.at[0])
    own_x.start()
    for a in range(3):
        own_copy(a).start()

    rows_all = arr.shape[0]
    M = min(256, rows_all)

    def multiply(a, src, first):
        acc = (gacc, uacc)[a]
        deep = pl.ds(pl.multiple_of(src * R, R), R)

        @pl.loop(0, rows_all // M)
        def _(m):
            rows = pl.ds(pl.multiple_of(m * M, M), M)
            value = jnp.dot(arr[rows, deep], wins[a][deep, :], preferred_element_type=jnp.float32)
            if first:
                acc[rows, :] = value
            else:
                acc[rows, :] += value

    def activate():
        @pl.loop(0, rows_all // 64)
        def _(m):
            rows = pl.ds(pl.multiple_of(m * 64, 64), 64)
            v = gacc[rows, :]
            hid[rows, :] = (v / (1.0 + jnp.exp(-v)) * uacc[rows, :]).astype(jnp.bfloat16)

    def partial_out(src, half):
        cols = cols_of(src, half)

        @pl.loop(0, rows_all // M)
        def _(m):
            rows = pl.ds(pl.multiple_of(m * M, M), M)
            pbf[rows, cols] = jnp.dot(hid[rows, :], dw[:, cols], preferred_element_type=jnp.float32).astype(jnp.bfloat16)

        for p in peers:
            p_copy(src, half, p, t).start()
        ret[slots(t), cols] = pbf[slots(t), cols]

    def mix(src, half, own):
        cols = cols_of(src, half)
        for p in peers:
            p_copy(src, half, p, p).wait_recv()
        value = jnp.dot(bh[...], ret[:, cols], preferred_element_type=jnp.float32) + jnp.dot(
            bl[...], ret[:, cols], preferred_element_type=jnp.float32)
        if own:
            mown[:, pl.ds(pl.multiple_of(half * H, H), H)] = value
        else:
            msend[:, cols] = value.astype(jnp.bfloat16)
            m_copy(src, half, f).start()

    own_x.wait()
    for p in peers:
        t_copy(p, p).wait_recv()
    for a in (0, 1):
        own_copy(a).wait()
        out_copy(a, f).start()
        multiply(a, f, True)
    own_copy(2).wait()
    out_copy(2, f).start()

    pending = []

    def submit(src, half, own):
        partial_out(src, half)
        pending.append((src, half, own))
        if len(pending) > 1:
            mix(*pending.pop(0))

    def finish(a, src):
        y_copy(a, src, 1 - g).wait_recv()
        out_copy(a, src).start()
        if a < 2:
            multiply(a, src, False)
        else:
            submit(src, 1 - g, False)

    items = [(a, src) for a in (0, 1) for src in others] + [(2, src) for src in others]
    last = None
    for i, (a, src) in enumerate(items):
        z_recv(a, src).wait_recv()
        y_copy(a, src, g).start()
        if last is not None:
            finish(*last)
            if i == 2 * len(others):
                activate()
                submit(f, 0, True)
                submit(f, 1, True)
        if a == 2:
            submit(src, g, False)
        last = (a, src)
    finish(*last)
    for entry in pending:
        mix(*entry)
    total = mown[...]
    for p in others:
        for half in range(2):
            m_copy(p, half, p).wait_recv()
        total = total + mrecv[p].astype(jnp.float32)
    mo[...] = total.astype(jnp.bfloat16)

    for p in peers:
        t_copy(p, t).wait_send()
        for c in range(F):
            for half in range(2):
                p_copy(c, half, p, t).wait_send()
    for p in others:
        for a in range(3):
            z_copy(a, p, f).wait_send()
            y_copy(a, p, g).wait_send()
        for half in range(2):
            m_copy(p, half, f).wait_send()
    for a in range(3):
        for c in range(F):
            out_copy(a, c).wait()


def exchange(F, T, gl, ul, dl, xs, bh, bl):
    R, FF = gl.shape
    C = FF // F
    D = F * R
    S = xs.shape[0] * xs.shape[1]
    tok = bh.shape[0]
    bf, f32 = jnp.bfloat16, jnp.float32
    any_spec, vm = pl.BlockSpec(memory_space=pl.ANY), pl.BlockSpec(memory_space=pltpu.VMEM)
    dma = pltpu.SemaphoreType.DMA
    return pl.pallas_call(
        functools.partial(exchange_kernel, F, T, R, C),
        name="exchange",
        out_shape=(jax.ShapeDtypeStruct((D, C), bf), jax.ShapeDtypeStruct((D, C), bf),
                   jax.ShapeDtypeStruct((C, D), bf), jax.ShapeDtypeStruct((tok, R), bf)),
        in_specs=[any_spec] * 4 + [vm] * 2,
        out_specs=(any_spec, any_spec, any_spec, vm),
        scratch_shapes=[
            pltpu.VMEM((D, C), bf), pltpu.VMEM((D, C), bf), pltpu.VMEM((C, D), bf), pltpu.VMEM((S, D), bf),
            pltpu.VMEM((S, C), f32), pltpu.VMEM((S, C), f32), pltpu.VMEM((S, C), bf),
            pltpu.VMEM((S, D), bf), pltpu.VMEM((S, D), bf), pltpu.VMEM((tok, D), bf),
            pltpu.VMEM((tok, R), f32), pltpu.VMEM((F, tok, R), bf),
            dma((3, F)), dma((3, F)), dma((3, F)), dma((3, F)), dma((T,)), dma((T,)),
            dma((F, 2, T)), dma((F, 2, T)), dma((F, 2)), dma((F, 2)), dma((3,)), dma((1,)), dma((3, F)),
        ],
        compiler_params=pltpu.CompilerParams(collective_id=0, has_side_effects=True, vmem_limit_bytes=60 * 1024 * 1024),
    )(gl, ul, dl, xs, bh, bl)


def fits(grp_count, fs_count, pieces, gate_train):
    rows, wide = gate_train.shape[1:]
    return (grp_count == 2 and fs_count == pieces and fs_count % 2 == 0
            and wide % (fs_count * 128) == 0 and rows % 256 == 0)


def swapped(gate_low, up_low, down_low, copies):
    gate_wide = jnp.tile(gate_low, (1, copies))
    up_wide = jnp.tile(up_low, (1, copies))
    down_wide = jnp.tile(down_low, (copies, 1))
    gate_new, up_new = (
        lax.all_to_all(gate_wide, "fs", split_axis=1, concat_axis=0, tiled=True),
        lax.all_to_all(up_wide, "fs", split_axis=1, concat_axis=0, tiled=True),
    )
    down_new = lax.all_to_all(down_wide, "fs", split_axis=0, concat_axis=1, tiled=True)
    return gate_new, up_new, down_new


def shards(tokens, routes, route_weight, norm_gain, gate_train, up_train, down_train):
    fs_count = lax.axis_size("fs")
    pieces = min(fs_count, 32)
    copies = fs_count // pieces
    gain_column = norm_gain[:, None]
    gate_low = (gate_train[0] * gain_column).astype(jnp.bfloat16)
    up_low = (up_train[0] * gain_column).astype(jnp.bfloat16)
    down_low = down_train[0].astype(jnp.bfloat16)
    fused = fits(lax.axis_size("grp"), fs_count, pieces, gate_train)
    if not fused:
        gate_new, up_new, down_new = swapped(gate_low, up_low, down_low, copies)
    tok_float = tokens.astype(jnp.float32)
    normed = (
        tok_float * lax.rsqrt(jnp.mean(tok_float * tok_float, axis=-1, keepdims=True) + 1e-06)
    ).astype(jnp.bfloat16)
    chosen = routes.reshape(-1)
    chosen_hot = (chosen[:, None] == jnp.arange(EXPERTS, dtype=jnp.int32)[None, :]).astype(
        jnp.int32
    )
    before = jnp.cumsum(chosen_hot, axis=0) - chosen_hot
    slot_rank = jnp.sum(before * chosen_hot, axis=1)
    slot_index = (chosen * CAP + slot_rank).reshape(routes.shape)
    slot_range = jnp.arange(EXPERTS * CAP, dtype=jnp.int32)
    select_rows = jnp.any(slot_range[:, None, None] == slot_index[None, :, :], axis=-1).astype(
        jnp.bfloat16
    )
    outgoing = jnp.dot(select_rows, normed, preferred_element_type=jnp.float32).astype(jnp.bfloat16)
    outgoing = outgoing.reshape(EXPERTS, CAP, normed.shape[1])
    blend_weight = jnp.sum(
        jnp.where(
            slot_range[None, None, :] == slot_index[:, :, None], route_weight[:, :, None], 0.0
        ),
        axis=1,
    )
    if fused:
        blend_high = lax.reduce_precision(blend_weight, 8, 7)
        blend_low = (blend_weight - blend_high).astype(jnp.bfloat16)
        blend_high = blend_high.astype(jnp.bfloat16)
        gate_new, up_new, down_new, mixed = exchange(
            fs_count, lax.axis_size("tp"), gate_low, up_low, down_low, outgoing, blend_high, blend_low
        )
        return (gate_new[None], up_new[None], down_new[None], mixed)
    arrived = lax.all_to_all(outgoing, "tp", split_axis=0, concat_axis=0, tiled=True).reshape(
        EXPERTS * CAP, normed.shape[1]
    )
    slot_count = EXPERTS * CAP // copies
    copy_index = lax.axis_index("fs") // pieces
    my_rows = lax.dynamic_slice_in_dim(arrived, copy_index * slot_count, slot_count, 0)
    gated = jnp.dot(my_rows, gate_new, preferred_element_type=jnp.float32)
    lifted = jnp.dot(my_rows, up_new, preferred_element_type=jnp.float32)
    hidden = (jax.nn.silu(gated) * lifted).astype(jnp.bfloat16)
    partial_out = jnp.dot(hidden, down_new, preferred_element_type=jnp.float32)
    placed = jnp.zeros((EXPERTS * CAP, partial_out.shape[1]), jnp.float32)
    placed = lax.dynamic_update_slice_in_dim(placed, partial_out, copy_index * slot_count, 0)
    expert_out = lax.psum_scatter(placed, "fs", scatter_dimension=1, tiled=True).astype(
        jnp.bfloat16
    )
    returned = lax.all_to_all(
        expert_out.reshape(EXPERTS, CAP, expert_out.shape[1]),
        "tp",
        split_axis=0,
        concat_axis=0,
        tiled=True,
    )
    returned = returned.reshape(EXPERTS * CAP, expert_out.shape[1]).astype(jnp.float32)
    mixed = jnp.dot(
        blend_weight, returned, precision=lax.Precision.HIGHEST, preferred_element_type=jnp.float32
    )
    return (gate_new[None], up_new[None], down_new[None], mixed.astype(jnp.bfloat16))


def solution(mesh):
    in_specs = (
        P(("grp", "tp"), None),
        P(("grp", "tp"), None),
        P(("grp", "tp"), None),
        P("fs"),
        P("tp", "fs", None),
        P("tp", "fs", None),
        P("tp", None, "fs"),
    )
    out_specs = (
        P(("grp", "tp"), None, "fs"),
        P(("grp", "tp"), None, "fs"),
        P(("grp", "tp"), "fs", None),
        P(("grp", "tp"), "fs"),
    )
    return jax.shard_map(shards, mesh=mesh, in_specs=in_specs, out_specs=out_specs, check_vma=False)
```

```python
import functools
import jax
import jax.numpy as jnp
from jax import lax
from jax.experimental import pallas as pl
from jax.experimental.pallas import tpu as pltpu
from jax.sharding import PartitionSpec as P

EXPERTS = 4
CAP = 128
MESH = pl.DeviceIdType.MESH


def exchange_kernel(F, T, R, C, Q, gt, ut, dt, gain, tokens, routes, routes_t, weight, gw, uw, dw, mo,
                    wide, tall, sendw, sendt, normed, xs, bh, bl,
                    arr, gacc, uacc, hid, pbf, ret, msend, mown, mrecv,
                    zs, zr, ys, yr, ts, tr, ps, pr, ms, mr, loc):
    g, f, t = lax.axis_index("grp"), lax.axis_index("fs"), lax.axis_index("tp")
    H = R // 2
    wins = (gw, uw, dw)
    pieces_of = (1, 1, Q)
    half_f = F // 2
    lo = lax.div(f, half_f)
    peers = [lax.rem(t + d, T) for d in range(1, T)]
    others = [lo * k + (1 - lo) * (F - 1 - k) for k in range(half_f)]
    others += [lo * half_f + lax.rem(f - lo * half_f + 1 + j, half_f) for j in range(half_f - 1)]

    barrier = pltpu.get_barrier_semaphore()
    for p in peers:
        pl.semaphore_signal(barrier, inc=1, device_id={"tp": p}, device_id_type=MESH)
    for p in others:
        pl.semaphore_signal(barrier, inc=1, device_id={"fs": p}, device_id_type=MESH)
    pl.semaphore_signal(barrier, inc=1, device_id={"grp": 1 - g}, device_id_type=MESH)
    pl.semaphore_wait(barrier, len(peers) + len(others) + 1)

    def cols_of(src, half):
        return pl.ds(pl.multiple_of(src * R + half * H, H), H)

    def part(a, src, half, q):
        if a < 2:
            return wins[a].at[cols_of(src, half), :]
        return dw.at[pl.ds(q * (C // Q), C // Q), cols_of(src, half)]

    def z_copy(a, k, tgt, src, q):
        piece = sendw.at[a, k] if a < 2 else sendt.at[k, pl.ds(q * (C // Q), C // Q), :]
        return pltpu.make_async_remote_copy(
            src_ref=piece, dst_ref=part(a, src, g, q), send_sem=zs.at[a, k, q], recv_sem=zr.at[a, src, q],
            device_id={"fs": tgt}, device_id_type=MESH)

    def z_send(a, k):
        for q in range(pieces_of[a]):
            z_copy(a, k, others[k], f, q).start()

    def z_recv(a, src, q):
        return pltpu.make_async_remote_copy(
            src_ref=part(a, src, g, q), dst_ref=part(a, src, g, q), send_sem=zs.at[a, 0, q],
            recv_sem=zr.at[a, src, q], device_id={"fs": src}, device_id_type=MESH)

    def y_copy(a, src, half, q):
        return pltpu.make_async_remote_copy(
            src_ref=part(a, src, half, q), dst_ref=part(a, src, half, q), send_sem=ys.at[a, src, q],
            recv_sem=yr.at[a, src, q], device_id={"grp": 1 - g}, device_id_type=MESH)

    def slots(q):
        return pl.ds(pl.multiple_of(q * CAP, CAP), CAP)

    def t_copy(tgt, src):
        return pltpu.make_async_remote_copy(
            src_ref=xs.at[slots(tgt), :], dst_ref=arr.at[slots(src), :], send_sem=ts.at[tgt], recv_sem=tr.at[src],
            device_id={"tp": tgt}, device_id_type=MESH)

    def p_copy(c, half, tgt, src):
        cols = cols_of(c, half)
        return pltpu.make_async_remote_copy(
            src_ref=pbf.at[slots(tgt), cols], dst_ref=ret.at[slots(src), cols],
            send_sem=ps.at[c, half, tgt], recv_sem=pr.at[c, half, src],
            device_id={"tp": tgt}, device_id_type=MESH)

    def m_copy(tgt, half, src):
        return pltpu.make_async_remote_copy(
            src_ref=msend.at[:, cols_of(tgt, half)], dst_ref=mrecv.at[src, :, pl.ds(pl.multiple_of(half * H, H), H)],
            send_sem=ms.at[tgt, half], recv_sem=mr.at[src, half],
            device_id={"fs": tgt}, device_id_type=MESH)

    tasks = [(a, k, g) for a in range(3) for k in range(len(others))]
    tasks += [(a, None, half) for a in range(3) for half in range(2)]

    def stage_copy(n):
        a, k, half = tasks[n]
        tgt = f if k is None else others[k]
        near, far = pl.ds(pl.multiple_of(half * H, H), H), pl.ds(pl.multiple_of(tgt * C, C), C)
        if a < 2:
            return pltpu.make_async_copy((gt, ut)[a].at[near, far], wide.at[n % 3], loc.at[n % 3])
        return pltpu.make_async_copy(dt.at[far, near], tall.at[n % 3], loc.at[3 + n % 3])

    def cast(n):
        a, k, half = tasks[n]
        stage_copy(n).wait()
        if a < 2:
            @pl.loop(0, H // 32)
            def _(m):
                rows = pl.ds(pl.multiple_of(m * 32, 32), 32)
                scale = gain[pl.ds(pl.multiple_of(half * H + m * 32, 32), 32), :]
                value = (wide[n % 3, rows, :] * scale).astype(jnp.bfloat16)
                if k is None:
                    wins[a][pl.ds(pl.multiple_of(f * R + half * H + m * 32, 32), 32), :] = value
                else:
                    sendw[a, k, rows, :] = value
        else:
            @pl.loop(0, C // 128)
            def _(m):
                rows = pl.ds(pl.multiple_of(m * 128, 128), 128)
                value = tall[n % 3, rows, :].astype(jnp.bfloat16)
                if k is None:
                    dw[rows, cols_of(f, half)] = value
                else:
                    sendt[k, rows, :] = value
        if n + 3 < len(tasks):
            stage_copy(n + 3).start()

    def route():
        tok, slot_all = tokens.shape[0], arr.shape[0]

        @pl.loop(0, tok // 32)
        def _(m):
            rows = pl.ds(pl.multiple_of(m * 32, 32), 32)
            value = tokens[rows, :].astype(jnp.float32)
            normed[rows, :] = (
                value * lax.rsqrt(jnp.mean(value * value, axis=-1, keepdims=True) + 1e-06)
            ).astype(jnp.bfloat16)

        def ranks(shape, axis, one, two, hot_first, earlier):
            expert = lax.broadcasted_iota(jnp.int32, shape, axis)
            hot = jnp.where((expert == one) | (expert == two), 1.0, 0.0).astype(jnp.bfloat16)
            order = (hot, earlier) if hot_first else (earlier, hot)
            before = jnp.dot(*order, preferred_element_type=jnp.float32)
            return [
                name.astype(jnp.float32) * CAP
                + jnp.sum(jnp.where(expert == name, before, 0.0), axis=axis, keepdims=True)
                for name in (one, two)
            ]

        row = lax.broadcasted_iota(jnp.int32, (tok, tok), 0)
        col = lax.broadcasted_iota(jnp.int32, (tok, tok), 1)
        first, second = ranks((16, tok), 0, routes_t[0:1, :], routes_t[1:2, :], True,
                              jnp.where(row < col, 1.0, 0.0).astype(jnp.bfloat16))
        slot = lax.broadcasted_iota(jnp.int32, (slot_all, tok), 0).astype(jnp.float32)
        select = jnp.where((slot == first) | (slot == second), 1.0, 0.0).astype(jnp.bfloat16)
        for n in range(4):
            cols = pl.ds(n * (F * R // 4), F * R // 4)
            xs[:, cols] = jnp.dot(select, normed[:, cols], preferred_element_type=jnp.float32).astype(jnp.bfloat16)
        first, second = ranks((tok, 128), 1, routes[:, 0:1], routes[:, 1:2], False,
                              jnp.where(row > col, 1.0, 0.0).astype(jnp.bfloat16))
        slot = lax.broadcasted_iota(jnp.int32, (tok, slot_all), 1).astype(jnp.float32)
        blend = jnp.where(slot == first, weight[:, 0:1], 0.0) + jnp.where(slot == second, weight[:, 1:2], 0.0)
        high = blend.astype(jnp.bfloat16)
        bh[...] = high
        bl[...] = (blend - high.astype(jnp.float32)).astype(jnp.bfloat16)

    for n in range(3):
        stage_copy(n).start()
    remote = 3 * len(others)
    for n in range(remote):
        cast(n)
        if n > 0:
            z_send(*tasks[n - 1][:2])
    route()
    z_send(*tasks[remote - 1][:2])
    for n in range(remote, len(tasks)):
        cast(n)
        if n == remote:
            for p in peers:
                t_copy(p, t).start()
    arr[slots(t), :] = xs[slots(t), :]

    rows_all = arr.shape[0]
    M = min(256, rows_all)

    def multiply(a, src, first):
        acc = (gacc, uacc)[a]
        deep = pl.ds(pl.multiple_of(src * R, R), R)

        @pl.loop(0, rows_all // M)
        def _(m):
            rows = pl.ds(pl.multiple_of(m * M, M), M)
            value = jnp.dot(arr[rows, deep], wins[a][deep, :], preferred_element_type=jnp.float32)
            if first:
                acc[rows, :] = value
            else:
                acc[rows, :] += value

    def activate():
        @pl.loop(0, rows_all // 64)
        def _(m):
            rows = pl.ds(pl.multiple_of(m * 64, 64), 64)
            v = gacc[rows, :]
            hid[rows, :] = (v / (1.0 + jnp.exp(-v)) * uacc[rows, :]).astype(jnp.bfloat16)

    def partial_out(src, half):
        cols = cols_of(src, half)

        @pl.loop(0, rows_all // M)
        def _(m):
            rows = pl.ds(pl.multiple_of(m * M, M), M)
            pbf[rows, cols] = jnp.dot(hid[rows, :], dw[:, cols], preferred_element_type=jnp.float32).astype(jnp.bfloat16)

        for p in peers:
            p_copy(src, half, p, t).start()
        ret[slots(t), cols] = pbf[slots(t), cols]

    def mix(src, half, own):
        cols = cols_of(src, half)
        for p in peers:
            p_copy(src, half, p, p).wait_recv()
        value = jnp.dot(bh[...], ret[:, cols], preferred_element_type=jnp.float32) + jnp.dot(
            bl[...], ret[:, cols], preferred_element_type=jnp.float32)
        if own:
            mown[:, pl.ds(pl.multiple_of(half * H, H), H)] = value
        else:
            msend[:, cols] = value.astype(jnp.bfloat16)
            m_copy(src, half, f).start()

    for p in peers:
        t_copy(p, p).wait_recv()
    for a in (0, 1):
        multiply(a, f, True)

    pending = []

    def submit(src, half, own):
        partial_out(src, half)
        pending.append((src, half, own))
        if len(pending) > 1:
            mix(*pending.pop(0))

    def finish(a, src):
        for q in range(pieces_of[a]):
            y_copy(a, src, 1 - g, q).wait_recv()
        if a < 2:
            multiply(a, src, False)
        else:
            submit(src, 1 - g, False)

    items = [(a, src) for a in (0, 1) for src in others] + [(2, src) for src in others]
    last = None
    for i, (a, src) in enumerate(items):
        for q in range(pieces_of[a]):
            z_recv(a, src, q).wait_recv()
            y_copy(a, src, g, q).start()
        if last is not None:
            finish(*last)
            if i == 2 * len(others):
                activate()
                submit(f, 0, True)
                submit(f, 1, True)
        if a == 2:
            submit(src, g, False)
        last = (a, src)
    finish(*last)
    for entry in pending:
        mix(*entry)
    total = mown[...]
    for p in others:
        for half in range(2):
            m_copy(p, half, p).wait_recv()
        total = total + mrecv[p].astype(jnp.float32)
    mo[...] = total.astype(jnp.bfloat16)

    for p in peers:
        t_copy(p, t).wait_send()
        for c in range(F):
            for half in range(2):
                p_copy(c, half, p, t).wait_send()
    for k, p in enumerate(others):
        for a in range(3):
            for q in range(pieces_of[a]):
                z_copy(a, k, p, f, q).wait_send()
                y_copy(a, p, g, q).wait_send()
        for half in range(2):
            m_copy(p, half, f).wait_send()


def exchange(F, T, gate, up, down, gain, tokens, routes, weight):
    R, FF = gate.shape
    C, D, H = FF // F, F * R, R // 2
    Q = 4
    tok, S = tokens.shape[0], EXPERTS * CAP
    bf, f32 = jnp.bfloat16, jnp.float32
    any_spec, vm = pl.BlockSpec(memory_space=pl.ANY), pl.BlockSpec(memory_space=pltpu.VMEM)
    dma = pltpu.SemaphoreType.DMA
    return pl.pallas_call(
        functools.partial(exchange_kernel, F, T, R, C, Q),
        name="exchange",
        out_shape=(pltpu.VMEM((D, C), bf), pltpu.VMEM((D, C), bf),
                   pltpu.VMEM((C, D), bf), jax.ShapeDtypeStruct((tok, R), bf)),
        in_specs=[any_spec] * 3 + [vm] * 5,
        out_specs=(vm, vm, vm, vm),
        scratch_shapes=[
            pltpu.VMEM((3, H, C), f32), pltpu.VMEM((3, C, H), f32),
            pltpu.VMEM((2, F - 1, H, C), bf), pltpu.VMEM((F - 1, C, H), bf),
            pltpu.VMEM((tok, D), bf), pltpu.VMEM((S, D), bf), pltpu.VMEM((tok, S), bf), pltpu.VMEM((tok, S), bf),
            pltpu.VMEM((S, D), bf),
            pltpu.VMEM((S, C), f32), pltpu.VMEM((S, C), f32), pltpu.VMEM((S, C), bf),
            pltpu.VMEM((S, D), bf), pltpu.VMEM((S, D), bf), pltpu.VMEM((tok, D), bf),
            pltpu.VMEM((tok, R), f32), pltpu.VMEM((F, tok, R), bf),
            dma((3, F, Q)), dma((3, F, Q)), dma((3, F, Q)), dma((3, F, Q)), dma((T,)), dma((T,)),
            dma((F, 2, T)), dma((F, 2, T)), dma((F, 2)), dma((F, 2)), dma((6,)),
        ],
        compiler_params=pltpu.CompilerParams(collective_id=0, has_side_effects=True, vmem_limit_bytes=42 * 1024 * 1024),
    )(gate, up, down, gain[:, None], tokens, routes, routes.T, weight)


def fits(grp_count, fs_count, pieces, gate_train):
    rows, wide = gate_train.shape[1:]
    return (grp_count == 2 and fs_count == pieces and fs_count % 2 == 0
            and wide % (fs_count * 128) == 0 and rows % 256 == 0 and 4 <= 2 * fs_count <= 8)


def shards(tokens, routes, route_weight, norm_gain, gate_train, up_train, down_train):
    fs_count = lax.axis_size("fs")
    pieces = min(fs_count, 32)
    copies = fs_count // pieces
    if fits(lax.axis_size("grp"), fs_count, pieces, gate_train):
        gate_new, up_new, down_new, mixed = exchange(
            fs_count, lax.axis_size("tp"), gate_train[0], up_train[0], down_train[0],
            norm_gain, tokens, routes, route_weight,
        )
        return (gate_new[None], up_new[None], down_new[None], mixed)
    gain_column = norm_gain[:, None]
    gate_low = (gate_train[0] * gain_column).astype(jnp.bfloat16)
    up_low = (up_train[0] * gain_column).astype(jnp.bfloat16)
    down_low = down_train[0].astype(jnp.bfloat16)
    gate_wide = jnp.tile(gate_low, (1, copies))
    up_wide = jnp.tile(up_low, (1, copies))
    down_wide = jnp.tile(down_low, (copies, 1))
    gate_new, up_new = (
        lax.all_to_all(gate_wide, "fs", split_axis=1, concat_axis=0, tiled=True),
        lax.all_to_all(up_wide, "fs", split_axis=1, concat_axis=0, tiled=True),
    )
    down_new = lax.all_to_all(down_wide, "fs", split_axis=0, concat_axis=1, tiled=True)
    tok_float = tokens.astype(jnp.float32)
    normed = (
        tok_float * lax.rsqrt(jnp.mean(tok_float * tok_float, axis=-1, keepdims=True) + 1e-06)
    ).astype(jnp.bfloat16)
    chosen = routes.reshape(-1)
    chosen_hot = (chosen[:, None] == jnp.arange(EXPERTS, dtype=jnp.int32)[None, :]).astype(
        jnp.int32
    )
    before = jnp.cumsum(chosen_hot, axis=0) - chosen_hot
    slot_rank = jnp.sum(before * chosen_hot, axis=1)
    slot_index = (chosen * CAP + slot_rank).reshape(routes.shape)
    slot_range = jnp.arange(EXPERTS * CAP, dtype=jnp.int32)
    select_rows = jnp.any(slot_range[:, None, None] == slot_index[None, :, :], axis=-1).astype(
        jnp.bfloat16
    )
    outgoing = jnp.dot(select_rows, normed, preferred_element_type=jnp.float32).astype(jnp.bfloat16)
    outgoing = outgoing.reshape(EXPERTS, CAP, normed.shape[1])
    arrived = lax.all_to_all(outgoing, "tp", split_axis=0, concat_axis=0, tiled=True).reshape(
        EXPERTS * CAP, normed.shape[1]
    )
    slot_count = EXPERTS * CAP // copies
    copy_index = lax.axis_index("fs") // pieces
    my_rows = lax.dynamic_slice_in_dim(arrived, copy_index * slot_count, slot_count, 0)
    gated = jnp.dot(my_rows, gate_new, preferred_element_type=jnp.float32)
    lifted = jnp.dot(my_rows, up_new, preferred_element_type=jnp.float32)
    hidden = (jax.nn.silu(gated) * lifted).astype(jnp.bfloat16)
    partial_out = jnp.dot(hidden, down_new, preferred_element_type=jnp.float32)
    placed = jnp.zeros((EXPERTS * CAP, partial_out.shape[1]), jnp.float32)
    placed = lax.dynamic_update_slice_in_dim(placed, partial_out, copy_index * slot_count, 0)
    expert_out = lax.psum_scatter(placed, "fs", scatter_dimension=1, tiled=True).astype(
        jnp.bfloat16
    )
    returned = lax.all_to_all(
        expert_out.reshape(EXPERTS, CAP, expert_out.shape[1]),
        "tp",
        split_axis=0,
        concat_axis=0,
        tiled=True,
    )
    returned = returned.reshape(EXPERTS * CAP, expert_out.shape[1]).astype(jnp.float32)
    blend_weight = jnp.sum(
        jnp.where(
            slot_range[None, None, :] == slot_index[:, :, None], route_weight[:, :, None], 0.0
        ),
        axis=1,
    )
    mixed = jnp.dot(
        blend_weight, returned, precision=lax.Precision.HIGHEST, preferred_element_type=jnp.float32
    )
    return (gate_new[None], up_new[None], down_new[None], mixed.astype(jnp.bfloat16))


def solution(mesh):
    in_specs = (
        P(("grp", "tp"), None),
        P(("grp", "tp"), None),
        P(("grp", "tp"), None),
        P("fs"),
        P("tp", "fs", None),
        P("tp", "fs", None),
        P("tp", None, "fs"),
    )
    out_specs = (
        P(("grp", "tp"), None, "fs"),
        P(("grp", "tp"), None, "fs"),
        P(("grp", "tp"), "fs", None),
        P(("grp", "tp"), "fs"),
    )
    return jax.shard_map(shards, mesh=mesh, in_specs=in_specs, out_specs=out_specs, check_vma=False)
```

```python
import functools
import jax
import jax.numpy as jnp
from jax import lax
from jax.experimental import pallas as pl
from jax.experimental.pallas import tpu as pltpu
from jax.sharding import PartitionSpec as P

EXPERTS = 4
CAP = 128
MESH = pl.DeviceIdType.MESH


def exchange_kernel(F, T, R, C, Q, gt, ut, dt, gain, tokens, routes_t, weight_t, gw, uw, dw, mo,
                    flat, turned, scale_at, wide, tall, sendw, sendt, normed, xs, bh, bl,
                    arr, gacc, uacc, hid, pbf, ret, msend, mown, mrecv,
                    zs, zr, ys, yr, ts, tr, ps, pr, ms, mr, loc):
    g, f, t = lax.axis_index("grp"), lax.axis_index("fs"), lax.axis_index("tp")
    H = R // 2
    wins = (gw, uw, dw)
    pieces_of = (1, 1, Q)
    half_f = F // 2
    lo = lax.div(f, half_f)
    peers = [lax.rem(t + d, T) for d in range(1, T)]
    others = [lo * k + (1 - lo) * (F - 1 - k) for k in range(half_f)]
    others += [lo * half_f + lax.rem(f - lo * half_f + 1 + j, half_f) for j in range(half_f - 1)]

    barrier = pltpu.get_barrier_semaphore()
    for p in peers:
        pl.semaphore_signal(barrier, inc=1, device_id={"tp": p}, device_id_type=MESH)
    for p in others:
        pl.semaphore_signal(barrier, inc=1, device_id={"fs": p}, device_id_type=MESH)
    pl.semaphore_signal(barrier, inc=1, device_id={"grp": 1 - g}, device_id_type=MESH)
    pl.semaphore_wait(barrier, len(peers) + len(others) + 1)

    def cols_of(src, half):
        return pl.ds(pl.multiple_of(src * R + half * H, H), H)

    def part(a, src, half, q):
        if a < 2:
            return wins[a].at[cols_of(src, half), :]
        return dw.at[pl.ds(q * (C // Q), C // Q), cols_of(src, half)]

    def z_copy(a, k, tgt, src, q):
        piece = sendw.at[a, k] if a < 2 else sendt.at[k, pl.ds(q * (C // Q), C // Q), :]
        return pltpu.make_async_remote_copy(
            src_ref=piece, dst_ref=part(a, src, g, q), send_sem=zs.at[a, k, q], recv_sem=zr.at[a, src, q],
            device_id={"fs": tgt}, device_id_type=MESH)

    def z_send(a, k):
        for q in range(pieces_of[a]):
            z_copy(a, k, others[k], f, q).start()

    def z_recv(a, src, q):
        return pltpu.make_async_remote_copy(
            src_ref=part(a, src, g, q), dst_ref=part(a, src, g, q), send_sem=zs.at[a, 0, q],
            recv_sem=zr.at[a, src, q], device_id={"fs": src}, device_id_type=MESH)

    def y_copy(a, src, half, q):
        return pltpu.make_async_remote_copy(
            src_ref=part(a, src, half, q), dst_ref=part(a, src, half, q), send_sem=ys.at[a, src, q],
            recv_sem=yr.at[a, src, q], device_id={"grp": 1 - g}, device_id_type=MESH)

    def slots(q):
        return pl.ds(pl.multiple_of(q * CAP, CAP), CAP)

    def t_copy(tgt, src):
        return pltpu.make_async_remote_copy(
            src_ref=xs.at[slots(tgt), :], dst_ref=arr.at[slots(src), :], send_sem=ts.at[tgt], recv_sem=tr.at[src],
            device_id={"tp": tgt}, device_id_type=MESH)

    def p_copy(c, half, tgt, src):
        cols = cols_of(c, half)
        return pltpu.make_async_remote_copy(
            src_ref=pbf.at[slots(tgt), cols], dst_ref=ret.at[slots(src), cols],
            send_sem=ps.at[c, half, tgt], recv_sem=pr.at[c, half, src],
            device_id={"tp": tgt}, device_id_type=MESH)

    def m_copy(tgt, half, src):
        return pltpu.make_async_remote_copy(
            src_ref=msend.at[:, cols_of(tgt, half)], dst_ref=mrecv.at[src, :, pl.ds(pl.multiple_of(half * H, H), H)],
            send_sem=ms.at[tgt, half], recv_sem=mr.at[src, half],
            device_id={"fs": tgt}, device_id_type=MESH)

    if len(others) == 3:
        order = [(0, 0), (0, 1), (0, 2), (1, 0), (1, 2), (2, 2), (1, 1), (2, 0), (2, 1)]
    else:
        order = [(a, k) for a in range(3) for k in range(len(others))]
    tasks = [(a, k, g) for a, k in order]
    tasks += [(a, None, half) for a in range(3) for half in range(2)]

    def stage_copy(n):
        a, k, half = tasks[n]
        tgt = f if k is None else others[k]
        near, far = pl.ds(pl.multiple_of(half * H, H), H), pl.ds(pl.multiple_of(tgt * C, C), C)
        if a < 2:
            return pltpu.make_async_copy((gt, ut)[a].at[near, far], wide.at[n % 3], loc.at[n % 3])
        return pltpu.make_async_copy(dt.at[far, near], tall.at[n % 3], loc.at[3 + n % 3])

    def cast(n):
        a, k, half = tasks[n]
        stage_copy(n).wait()
        if a < 2:
            @pl.loop(0, H // 32)
            def _(m):
                rows = pl.ds(pl.multiple_of(m * 32, 32), 32)
                scale = scale_at[pl.ds(pl.multiple_of(half * H + m * 32, 32), 32), 0:1]
                value = (wide[n % 3, rows, :] * scale).astype(jnp.bfloat16)
                if k is None:
                    wins[a][pl.ds(pl.multiple_of(f * R + half * H + m * 32, 32), 32), :] = value
                else:
                    sendw[a, k, rows, :] = value
        else:
            @pl.loop(0, C // 128)
            def _(m):
                rows = pl.ds(pl.multiple_of(m * 128, 128), 128)
                value = tall[n % 3, rows, :].astype(jnp.bfloat16)
                if k is None:
                    dw[rows, cols_of(f, half)] = value
                else:
                    sendt[k, rows, :] = value
        if n + 3 < len(tasks):
            stage_copy(n + 3).start()

    def route():
        tok, slot_all = tokens.shape[0], arr.shape[0]

        @pl.loop(0, tok // 32)
        def _(m):
            rows = pl.ds(pl.multiple_of(m * 32, 32), 32)
            value = tokens[rows, :].astype(jnp.float32)
            normed[rows, :] = (
                value * lax.rsqrt(jnp.mean(value * value, axis=-1, keepdims=True) + 1e-06)
            ).astype(jnp.bfloat16)

        one, two = routes_t[0:1, :], routes_t[1:2, :]
        row = lax.broadcasted_iota(jnp.int32, (tok, tok), 0)
        col = lax.broadcasted_iota(jnp.int32, (tok, tok), 1)
        expert = lax.broadcasted_iota(jnp.int32, (16, tok), 0)
        hot = jnp.where((expert == one) | (expert == two), 1.0, 0.0).astype(jnp.bfloat16)
        before = jnp.dot(hot, jnp.where(row < col, 1.0, 0.0).astype(jnp.bfloat16), preferred_element_type=jnp.float32)
        first, second = [
            name.astype(jnp.float32) * CAP
            + jnp.sum(jnp.where(expert == name, before, 0.0), axis=0, keepdims=True)
            for name in (one, two)
        ]
        slot = lax.broadcasted_iota(jnp.int32, (slot_all, tok), 0).astype(jnp.float32)
        select = jnp.where((slot == first) | (slot == second), 1.0, 0.0).astype(jnp.bfloat16)
        for n in range(4):
            cols = pl.ds(n * (F * R // 4), F * R // 4)
            xs[:, cols] = jnp.dot(select, normed[:, cols], preferred_element_type=jnp.float32).astype(jnp.bfloat16)
        flat[...] = jnp.zeros_like(flat)
        for n, line in enumerate((first, second, weight_t[0:1, :], weight_t[1:2, :])):
            flat[n:n + 1, 0:tok] = line
        turned[...] = flat[...].T
        slot = lax.broadcasted_iota(jnp.int32, (tok, slot_all), 1).astype(jnp.float32)
        blend = jnp.where(slot == turned[0:tok, 0:1], turned[0:tok, 2:3], 0.0) + jnp.where(
            slot == turned[0:tok, 1:2], turned[0:tok, 3:4], 0.0)
        high = blend.astype(jnp.bfloat16)
        bh[...] = high
        bl[...] = (blend - high.astype(jnp.float32)).astype(jnp.bfloat16)

    for n in range(3):
        stage_copy(n).start()
    for n in range(R // 128):
        piece = pl.ds(n * 128, 128)
        scale_at[piece, :] = jnp.broadcast_to(gain[0:1, piece], (128, 128)).T
    remote = 3 * len(others)
    for n in range(remote):
        cast(n)
        if n > 0:
            z_send(*tasks[n - 1][:2])
    route()
    z_send(*tasks[remote - 1][:2])
    for n in range(remote, len(tasks)):
        cast(n)
        if n == remote:
            for p in peers:
                t_copy(p, t).start()
    arr[slots(t), :] = xs[slots(t), :]

    rows_all = arr.shape[0]
    M = min(256, rows_all)

    def multiply(a, src, first):
        acc = (gacc, uacc)[a]
        deep = pl.ds(pl.multiple_of(src * R, R), R)

        @pl.loop(0, rows_all // M)
        def _(m):
            rows = pl.ds(pl.multiple_of(m * M, M), M)
            value = jnp.dot(arr[rows, deep], wins[a][deep, :], preferred_element_type=jnp.float32)
            if first:
                acc[rows, :] = value
            else:
                acc[rows, :] += value

    def activate():
        @pl.loop(0, rows_all // 64)
        def _(m):
            rows = pl.ds(pl.multiple_of(m * 64, 64), 64)
            v = gacc[rows, :]
            hid[rows, :] = (v / (1.0 + jnp.exp(-v)) * uacc[rows, :]).astype(jnp.bfloat16)

    def partial_out(src, half):
        cols = cols_of(src, half)

        @pl.loop(0, rows_all // M)
        def _(m):
            rows = pl.ds(pl.multiple_of(m * M, M), M)
            pbf[rows, cols] = jnp.dot(hid[rows, :], dw[:, cols], preferred_element_type=jnp.float32).astype(jnp.bfloat16)

        for p in peers:
            p_copy(src, half, p, t).start()
        ret[slots(t), cols] = pbf[slots(t), cols]

    def mix(src, half, own):
        cols = cols_of(src, half)
        for p in peers:
            p_copy(src, half, p, p).wait_recv()
        value = jnp.dot(bh[...], ret[:, cols], preferred_element_type=jnp.float32) + jnp.dot(
            bl[...], ret[:, cols], preferred_element_type=jnp.float32)
        if own:
            mown[:, pl.ds(pl.multiple_of(half * H, H), H)] = value
        else:
            msend[:, cols] = value.astype(jnp.bfloat16)
            m_copy(src, half, f).start()

    for p in peers:
        t_copy(p, p).wait_recv()
    for a in (0, 1):
        multiply(a, f, True)

    pending = []

    def submit(src, half, own):
        partial_out(src, half)
        pending.append((src, half, own))
        if len(pending) > 1:
            mix(*pending.pop(0))

    def finish(a, src):
        for q in range(pieces_of[a]):
            y_copy(a, src, 1 - g, q).wait_recv()
        if a < 2:
            multiply(a, src, False)
        else:
            offer(src, 1 - g)

    waiting, done = [], []

    def offer(src, half):
        waiting.append((src, half, False))
        if len(done) == 2 * len(others):
            while waiting:
                submit(*waiting.pop(0))

    def settle(a, src):
        finish(a, src)
        if a < 2:
            done.append(src)
            if len(done) == 2 * len(others):
                activate()
                submit(f, 0, True)
                submit(f, 1, True)

    items = [(a, others[k]) for a, k in order]
    last = None
    for a, src in items:
        for q in range(pieces_of[a]):
            z_recv(a, src, q).wait_recv()
            y_copy(a, src, g, q).start()
        if last is not None:
            settle(*last)
        if a == 2:
            offer(src, g)
        last = (a, src)
    settle(*last)
    for entry in pending:
        mix(*entry)
    total = mown[...]
    for p in others:
        for half in range(2):
            m_copy(p, half, p).wait_recv()
        total = total + mrecv[p].astype(jnp.float32)
    mo[...] = total.astype(jnp.bfloat16)

    for p in peers:
        t_copy(p, t).wait_send()
        for c in range(F):
            for half in range(2):
                p_copy(c, half, p, t).wait_send()
    for k, p in enumerate(others):
        for a in range(3):
            for q in range(pieces_of[a]):
                z_copy(a, k, p, f, q).wait_send()
                y_copy(a, p, g, q).wait_send()
        for half in range(2):
            m_copy(p, half, f).wait_send()


def exchange(F, T, gate, up, down, gain, tokens, routes, weight):
    span = -(-tokens.shape[0] // 128) * 128
    R, FF = gate.shape
    C, D, H = FF // F, F * R, R // 2
    Q = 4
    tok, S = tokens.shape[0], EXPERTS * CAP
    bf, f32 = jnp.bfloat16, jnp.float32
    any_spec, vm = pl.BlockSpec(memory_space=pl.ANY), pl.BlockSpec(memory_space=pltpu.VMEM)
    dma = pltpu.SemaphoreType.DMA
    return pl.pallas_call(
        functools.partial(exchange_kernel, F, T, R, C, Q),
        name="exchange",
        out_shape=(pltpu.VMEM((D, C), bf), pltpu.VMEM((D, C), bf),
                   pltpu.VMEM((C, D), bf), jax.ShapeDtypeStruct((tok, R), bf)),
        in_specs=[any_spec] * 3 + [vm] * 4,
        out_specs=(vm, vm, vm, vm),
        scratch_shapes=[
            pltpu.VMEM((128, span), f32), pltpu.VMEM((span, 128), f32), pltpu.VMEM((R, 128), f32),
            pltpu.VMEM((3, H, C), f32), pltpu.VMEM((3, C, H), f32),
            pltpu.VMEM((2, F - 1, H, C), bf), pltpu.VMEM((F - 1, C, H), bf),
            pltpu.VMEM((tok, D), bf), pltpu.VMEM((S, D), bf), pltpu.VMEM((tok, S), bf), pltpu.VMEM((tok, S), bf),
            pltpu.VMEM((S, D), bf),
            pltpu.VMEM((S, C), f32), pltpu.VMEM((S, C), f32), pltpu.VMEM((S, C), bf),
            pltpu.VMEM((S, D), bf), pltpu.VMEM((S, D), bf), pltpu.VMEM((tok, D), bf),
            pltpu.VMEM((tok, R), f32), pltpu.VMEM((F, tok, R), bf),
            dma((3, F, Q)), dma((3, F, Q)), dma((3, F, Q)), dma((3, F, Q)), dma((T,)), dma((T,)),
            dma((F, 2, T)), dma((F, 2, T)), dma((F, 2)), dma((F, 2)), dma((6,)),
        ],
        compiler_params=pltpu.CompilerParams(collective_id=0, has_side_effects=True, vmem_limit_bytes=42 * 1024 * 1024),
    )(gate, up, down, gain[None, :], tokens, routes.T, weight.T)


def fits(grp_count, fs_count, pieces, gate_train):
    rows, wide = gate_train.shape[1:]
    return (grp_count == 2 and fs_count == pieces and fs_count % 2 == 0
            and wide % (fs_count * 128) == 0 and rows % 256 == 0 and 4 <= 2 * fs_count <= 8)


def shards(tokens, routes, route_weight, norm_gain, gate_train, up_train, down_train):
    fs_count = lax.axis_size("fs")
    pieces = min(fs_count, 32)
    copies = fs_count // pieces
    if fits(lax.axis_size("grp"), fs_count, pieces, gate_train):
        gate_new, up_new, down_new, mixed = exchange(
            fs_count, lax.axis_size("tp"), gate_train[0], up_train[0], down_train[0],
            norm_gain, tokens, routes, route_weight,
        )
        return (gate_new[None], up_new[None], down_new[None], mixed)
    gain_column = norm_gain[:, None]
    gate_low = (gate_train[0] * gain_column).astype(jnp.bfloat16)
    up_low = (up_train[0] * gain_column).astype(jnp.bfloat16)
    down_low = down_train[0].astype(jnp.bfloat16)
    gate_wide = jnp.tile(gate_low, (1, copies))
    up_wide = jnp.tile(up_low, (1, copies))
    down_wide = jnp.tile(down_low, (copies, 1))
    gate_new, up_new = (
        lax.all_to_all(gate_wide, "fs", split_axis=1, concat_axis=0, tiled=True),
        lax.all_to_all(up_wide, "fs", split_axis=1, concat_axis=0, tiled=True),
    )
    down_new = lax.all_to_all(down_wide, "fs", split_axis=0, concat_axis=1, tiled=True)
    tok_float = tokens.astype(jnp.float32)
    normed = (
        tok_float * lax.rsqrt(jnp.mean(tok_float * tok_float, axis=-1, keepdims=True) + 1e-06)
    ).astype(jnp.bfloat16)
    chosen = routes.reshape(-1)
    chosen_hot = (chosen[:, None] == jnp.arange(EXPERTS, dtype=jnp.int32)[None, :]).astype(
        jnp.int32
    )
    before = jnp.cumsum(chosen_hot, axis=0) - chosen_hot
    slot_rank = jnp.sum(before * chosen_hot, axis=1)
    slot_index = (chosen * CAP + slot_rank).reshape(routes.shape)
    slot_range = jnp.arange(EXPERTS * CAP, dtype=jnp.int32)
    select_rows = jnp.any(slot_range[:, None, None] == slot_index[None, :, :], axis=-1).astype(
        jnp.bfloat16
    )
    outgoing = jnp.dot(select_rows, normed, preferred_element_type=jnp.float32).astype(jnp.bfloat16)
    outgoing = outgoing.reshape(EXPERTS, CAP, normed.shape[1])
    arrived = lax.all_to_all(outgoing, "tp", split_axis=0, concat_axis=0, tiled=True).reshape(
        EXPERTS * CAP, normed.shape[1]
    )
    slot_count = EXPERTS * CAP // copies
    copy_index = lax.axis_index("fs") // pieces
    my_rows = lax.dynamic_slice_in_dim(arrived, copy_index * slot_count, slot_count, 0)
    gated = jnp.dot(my_rows, gate_new, preferred_element_type=jnp.float32)
    lifted = jnp.dot(my_rows, up_new, preferred_element_type=jnp.float32)
    hidden = (jax.nn.silu(gated) * lifted).astype(jnp.bfloat16)
    partial_out = jnp.dot(hidden, down_new, preferred_element_type=jnp.float32)
    placed = jnp.zeros((EXPERTS * CAP, partial_out.shape[1]), jnp.float32)
    placed = lax.dynamic_update_slice_in_dim(placed, partial_out, copy_index * slot_count, 0)
    expert_out = lax.psum_scatter(placed, "fs", scatter_dimension=1, tiled=True).astype(
        jnp.bfloat16
    )
    returned = lax.all_to_all(
        expert_out.reshape(EXPERTS, CAP, expert_out.shape[1]),
        "tp",
        split_axis=0,
        concat_axis=0,
        tiled=True,
    )
    returned = returned.reshape(EXPERTS * CAP, expert_out.shape[1]).astype(jnp.float32)
    blend_weight = jnp.sum(
        jnp.where(
            slot_range[None, None, :] == slot_index[:, :, None], route_weight[:, :, None], 0.0
        ),
        axis=1,
    )
    mixed = jnp.dot(
        blend_weight, returned, precision=lax.Precision.HIGHEST, preferred_element_type=jnp.float32
    )
    return (gate_new[None], up_new[None], down_new[None], mixed.astype(jnp.bfloat16))


def solution(mesh):
    in_specs = (
        P(("grp", "tp"), None),
        P(("grp", "tp"), None),
        P(("grp", "tp"), None),
        P("fs"),
        P("tp", "fs", None),
        P("tp", "fs", None),
        P("tp", None, "fs"),
    )
    out_specs = (
        P(("grp", "tp"), None, "fs"),
        P(("grp", "tp"), None, "fs"),
        P(("grp", "tp"), "fs", None),
        P(("grp", "tp"), "fs"),
    )
    return jax.shard_map(shards, mesh=mesh, in_specs=in_specs, out_specs=out_specs, check_vma=False)
```
